32 devices in a mesh: sp: 16 (over z, y, x), tp: 2 (over core).
Axes of the slice: x: 2, y: 2, z: 4, core: 2. Of those that a mesh axis runs over, the one named last changes fastest.
Arguments:
- pool_input: bfloat16 [8192, 512], P('sp', 'tp'), may hold values from -8 to 8
- documents: int32 [8192], P('sp'), may hold values from 0 to 3, never falling along the last dimension, each value on 1 to 4096 neighbouring positions
- residual: bfloat16 [8192, 2048], P(('sp', 'tp')), may hold values from -6 to 6
- group_weights: bfloat16 [8, 64, 64], replicated, may hold values from -0.75 to 0.75
- pool_gain: bfloat16 [512], replicated, may hold values from 0.099609375 to 1.8984375
- output_weight: bfloat16 [512, 2048], replicated, may hold values from -0.25 to 0.25
- mixer_gain: bfloat16 [2048], replicated, may hold values from 0.099609375 to 1.8984375
- routed_gain: bfloat16 [2048], replicated, may hold values from 0.099609375 to 1.8984375
- final_gain: bfloat16 [2048], replicated, may hold values from 0.099609375 to 1.8984375
- chosen_group: int32 [8192, 1], P(('sp', 'tp')), may hold values from 0 to 15; in each aligned block of 256 rows (0 to 255, 256 to 511, ...) at most 32 rows name the same one
- chosen_experts: int32 [8192, 2], P(('sp', 'tp')), may hold values from 0 to 2, all different within a row
- expert_share: bfloat16 [8192, 2], P(('sp', 'tp')), may hold values from 0.099609375 to 1
- expert_gate: bfloat16 [48, 2048, 1024], P('sp', None, 'tp'), may hold values from -0.125 to 0.125
- expert_up: bfloat16 [48, 2048, 1024], P('sp', None, 'tp'), may hold values from -0.125 to 0.125
- expert_down: bfloat16 [48, 1024, 2048], P('sp', 'tp'), may hold values from -0.1875 to 0.1875
Outputs:
- updated: bfloat16 [8192, 2048], P(('sp', 'tp'))
The draws below stay inside these ranges and needn't reach their ends.
Inputs may be any that keep to these rules, and one draw needn't show every extreme that they name: `documents`: document numbers never fall along the sequence; every number appears, and a document holds 1 to 4096 positions. `chosen_group`: among the rows of one device at most 32 name the same group, and in every draw some group is named by exactly 32 rows of some device. `chosen_experts`: each row names 2 different experts of its group.
All inputs are finite; a program needn't handle non-finite values.
Results may differ from the reference program's by a relative error of at most 0.012.
Values may be sent and summed in bfloat16 or wider, within the bound.
A program may use at most 128 MiB of HBM per device.

```python
import math
import jax
import jax.numpy as jnp
import numpy as np
from jax import lax

D = 2048
POOL_GROUPS = 8
GROUP_DIM = 64
POOL_WIDTH = 512
FFE = 1024
EPG = 3
TOPK = 2
TOK_DEV = 512
TOKENS = 8192
ROWS = 256
HALO = 256
WIN_S = 128
WIN_M = 256
WIN_L = 512
DOCS = 4
DOC_MAX = 4096
GROUPS = 16
EXPERTS = 48
CAP = 32
FFE_PART = 512
N_TP = 2


def draw_pool_input(key, part):
    noise_key = jax.random.fold_in(key, 11)
    coarse_key = jax.random.fold_in(key, 12)
    fine_key = jax.random.fold_in(key, 13)
    coarse = jax.random.normal(coarse_key, (TOKENS // HALO, POOL_WIDTH), jnp.float32)
    fine = jax.random.normal(fine_key, (TOKENS // (TOK_DEV // 8), POOL_WIDTH), jnp.float32)
    offsets = jnp.repeat(coarse, HALO, axis=0) + 0.7 * jnp.repeat(fine, TOK_DEV // 8, axis=0)
    values = jax.random.normal(noise_key, (TOKENS, POOL_WIDTH), jnp.float32) + offsets
    return jnp.clip(values, -8.0, 8.0).astype(jnp.bfloat16)


def block_scale(key, shape, cuts, low, largest):
    level, own = 1.0, jax.random.fold_in(key, 6)
    for position, parts in cuts:
        draws = jnp.exp(jax.random.uniform(jax.random.fold_in(own, position), (parts,), jnp.float32, low / len(cuts), largest / len(cuts)))
        level = level * jnp.repeat(draws, shape[position] // parts).reshape([-1 if axis == position else 1 for axis in range(len(shape))])
    return level


def choose_distinct(rng, rows, number_of, top, lift):
    ranking = jax.random.permutation(jax.random.fold_in(rng, 1), number_of)
    favour = ranking
    for power in range(3):
        favour = favour * favour // number_of
    favour = favour * lift // number_of
    lots = jax.random.randint(jax.random.fold_in(rng, 2), (rows, number_of), 0, 4096) + favour
    fixed_rows = jax.random.permutation(jax.random.fold_in(rng, 3), rows)[jnp.arange(number_of) % rows]
    lots = jnp.where(jnp.arange(rows)[:, None] == fixed_rows[None, :], 1 << 14, lots)
    merit = lots * number_of + jnp.arange(number_of)
    return lax.top_k(merit.astype(jnp.int32), top)[1].astype(jnp.int32)


def profile(count, total, most, skew):
    portions = [(1 << 20) // math.isqrt(standing ** skew) + 1 for standing in range(2, count + 1)]
    spare, given = total - most - (count - 1), [1] * (count - 1)
    while spare > 0:
        free = [i for i in range(count - 1) if given[i] < most]
        pool, budget = sum([portions[i] for i in free]), spare
        for i in free:
            addition = min(most - given[i], max(1, budget * portions[i] // pool), spare)
            given[i] = given[i] + addition
            spare = spare - addition
    return np.array([most] + given)


def uneven(key, number_of, total, bound, skew):
    if number_of == 2:
        one = jax.random.randint(key, (), max(1, total - bound), min(bound, total - 1) + 1)
        return jnp.stack([one, total - one])
    sizes = jnp.asarray(profile(number_of, total, bound, skew), jnp.int32)
    twos = (number_of - 1) // 2
    donor, sink = sizes[1:1 + 2 * twos:2], sizes[2:2 + 2 * twos:2]
    margin = jnp.minimum(donor - 1, bound - sink)
    passed = jax.random.randint(jax.random.fold_in(key, 1), (twos,), 0, 1 << 20) % (margin + 1)
    sizes = sizes.at[1:1 + 2 * twos:2].set(donor - passed).at[2:2 + 2 * twos:2].set(sink + passed)
    return sizes[jax.random.permutation(jax.random.fold_in(key, 2), number_of)]


def routed_block(key, own, number, rows, count, top, limit, skew):
    ranking = jax.random.permutation(key, count)
    packed, common = portions_of(count, rows * top, limit, skew, True), portions_of(count, rows * top, limit, skew, False)
    places = jnp.arange(count)

    def named(tallies, offset_by):
        used = int((tallies > 0).sum())
        fixed = max(1, used // 4)
        passed = fixed + (places - fixed + offset_by * (used - fixed)) % max(1, count - fixed)
        return jnp.zeros((count,), jnp.int32).at[ranking[jnp.where(places < fixed, places, passed)]].set(jnp.asarray(tallies, jnp.int32))

    tallies = jnp.where(number % 4 == 0, named(packed, number // 4), named(common, number - number // 4 - 1))
    mixed = jax.random.permutation(jax.random.fold_in(own, 3), count)
    donor, sink = mixed[0:count // 2 * 2:2], mixed[1:count // 2 * 2:2]
    room = jnp.minimum(tallies[donor] - 1, limit - tallies[sink]) // 2
    room = jnp.where((donor == ranking[0]) | (sink == ranking[0]) | (tallies[sink] == 0), 0, jnp.maximum(room, 0))
    passed = jax.random.randint(jax.random.fold_in(own, 4), (count // 2,), 0, 1 << 20) % (room + 1)
    tallies = tallies.at[donor].add(-passed).at[sink].add(passed)
    items = jnp.searchsorted(jnp.cumsum(tallies), jnp.arange(rows * top), side="right").astype(jnp.int32)
    table = items.reshape(top, rows).T
    table = table[jax.random.permutation(jax.random.fold_in(own, 1), rows)]
    offset_by = jax.random.randint(jax.random.fold_in(own, 2), (rows, 1), 0, top)
    return jnp.take_along_axis(table, (jnp.arange(top)[None, :] + offset_by) % top, axis=1)


def portions_of(number_of, total, limit, lean, full):
    weights = [(1 << 20) // math.isqrt(grade ** lean) + 1 for grade in range(1, number_of + 1)]
    largest = limit if full else min(limit, max(-(-total // number_of), total * weights[0] // sum(weights)))
    least = 1 if total - largest >= number_of - 1 else 0
    counts, spare = [largest] + [least] * (number_of - 1), total - largest - least * (number_of - 1)
    while spare > 0:
        movable = [i for i in range(1, number_of) if counts[i] < largest] or [i for i in range(1, number_of) if counts[i] < limit]
        whole, left = sum([weights[i] for i in movable]), spare
        for i in movable:
            addition = min(limit - counts[i], max(1, left * weights[i] // whole), spare)
            counts[i] = counts[i] + addition
            spare = spare - addition
    return np.array(counts)


def bell_draw(own_key, extent, width, most, shards=(), kind=jnp.bfloat16):
    entries = jax.random.normal(own_key, extent, jnp.float32) * width
    if len(shards) > 0:
        entries = block_scale(own_key, extent, shards, -0.22, 0.18) * entries
    return jnp.clip(entries, min=-most, max=most).astype(kind)


def setup_inputs(seed: int = 0) -> dict:
    arg_keys = jax.random.split(jax.random.key(seed), 16)
    pool_input = draw_pool_input(jax.random.fold_in(arg_keys[15], 71), 0)
    documents = jnp.searchsorted(jnp.cumsum(uneven(arg_keys[1], DOCS, TOKENS, DOC_MAX, 2)), jnp.arange(TOKENS), side="right").astype(jnp.int32)
    residual = bell_draw(arg_keys[2], (TOKENS, D), 1.0, 6.0, ((0, 32),))
    group_weights = bell_draw(arg_keys[3], (POOL_GROUPS, GROUP_DIM, GROUP_DIM), GROUP_DIM ** -0.5, 0.75)
    pool_gain = jnp.clip(1.0 + 0.18 * jax.random.normal(arg_keys[4], (POOL_WIDTH,), jnp.float32), 0.099609375, 1.8984375).astype(jnp.bfloat16)
    output_weight = bell_draw(arg_keys[5], (POOL_WIDTH, D), POOL_WIDTH ** -0.5, 0.25)
    mixer_gain = jnp.clip(1.0 + 0.18 * jax.random.normal(arg_keys[6], (D,), jnp.float32), 0.099609375, 1.8984375).astype(jnp.bfloat16)
    routed_gain = jnp.clip(1.0 + 0.18 * jax.random.normal(arg_keys[7], (D,), jnp.float32), 0.099609375, 1.8984375).astype(jnp.bfloat16)
    final_gain = jnp.clip(1.0 + 0.18 * jax.random.normal(arg_keys[8], (D,), jnp.float32), 0.099609375, 1.8984375).astype(jnp.bfloat16)
    chosen_group_keys = jax.random.split(jax.random.fold_in(arg_keys[9], 1), TOKENS // ROWS)
    chosen_group_turns = jax.random.permutation(jax.random.fold_in(arg_keys[9], 3), TOKENS // ROWS)
    chosen_group = jax.vmap(lambda own, number: routed_block(jax.random.fold_in(arg_keys[9], 2), own, number, ROWS, GROUPS, 1, CAP, 1))(chosen_group_keys, chosen_group_turns).reshape((TOKENS, 1))
    chosen_experts = choose_distinct(arg_keys[10], TOKENS, EPG, TOPK, 0)
    expert_share = jnp.clip(0.099609375 + 0.9003906 * jax.random.uniform(arg_keys[11], (TOKENS, TOPK), jnp.float32) ** block_scale(arg_keys[11], (TOKENS, TOPK), ((0, 32),), -0.2, 0.2), 0.099609375, 1.0).astype(jnp.bfloat16)
    expert_gate = bell_draw(arg_keys[12], (EXPERTS, D, FFE), D ** -0.5, 0.125, ((0, 16), (2, 2)))
    expert_up = bell_draw(arg_keys[13], (EXPERTS, D, FFE), D ** -0.5, 0.125, ((0, 16), (2, 2)))
    expert_down = bell_draw(arg_keys[14], (EXPERTS, FFE, D), FFE ** -0.5, 0.1875, ((0, 16), (1, 2)))
    return {"pool_input": pool_input, "documents": documents, "residual": residual, "group_weights": group_weights, "pool_gain": pool_gain, "output_weight": output_weight, "mixer_gain": mixer_gain, "routed_gain": routed_gain, "final_gain": final_gain, "chosen_group": chosen_group, "chosen_experts": chosen_experts, "expert_share": expert_share, "expert_gate": expert_gate, "expert_up": expert_up, "expert_down": expert_down}


EPSILON = 1e-06
row_block = 64

def rms_scale(values, gain):
    return values * lax.rsqrt(lax.optimization_barrier(jnp.mean(values * values, axis=-1, keepdims=True)) + EPSILON) * gain.astype(jnp.float32)

def expert_rows(block_in, block_share, block_group, expert_gate, expert_up, expert_down):
    total = jnp.zeros(block_in.shape, jnp.float32)
    for block_part in range(N_TP):
        start = block_part * FFE_PART
        finish = start + FFE_PART
        part_sum = jnp.zeros(block_in.shape, jnp.float32)
        for expert in range(EPG):
            chosen = block_group * EPG + expert
            gate_full = lax.dynamic_index_in_dim(expert_gate, chosen, 0, keepdims=False)
            up_full = lax.dynamic_index_in_dim(expert_up, chosen, 0, keepdims=False)
            down_full = lax.dynamic_index_in_dim(expert_down, chosen, 0, keepdims=False)
            gate = jnp.dot(block_in, gate_full[:, start:finish], preferred_element_type=jnp.float32)
            upper = jnp.dot(block_in, up_full[:, start:finish], preferred_element_type=jnp.float32)
            hidden = (jax.nn.silu(gate) * upper).astype(jnp.bfloat16)
            product = jnp.dot(hidden, down_full[start:finish], preferred_element_type=jnp.float32)
            part_sum = part_sum + product * block_share[:, expert:expert + 1]
        total = total + lax.optimization_barrier(part_sum.astype(jnp.bfloat16)).astype(jnp.float32)
    return total.astype(jnp.bfloat16)

def reference(pool_input, documents, residual, group_weights, pool_gain, output_weight, mixer_gain, routed_gain, final_gain, chosen_group, chosen_experts, expert_share, expert_gate, expert_up, expert_down):
    values = pool_input.astype(jnp.float32)
    positions = jnp.arange(TOKENS, dtype=jnp.int32)
    doc_count = jax.ops.segment_sum(jnp.ones((TOKENS,), jnp.int32), documents, num_segments=DOCS)
    doc_begin = jnp.cumsum(doc_count) - doc_count
    begin = doc_begin[documents]
    finish = begin + doc_count[documents]
    doc_count_f = doc_count.astype(jnp.float32)
    prefix = jnp.concatenate([jnp.zeros((1, POOL_WIDTH), jnp.float32), jnp.cumsum(values, axis=0)], axis=0)
    windows = (WIN_S, WIN_M, WIN_L)
    pieces = []
    for group in range(POOL_GROUPS):
        start = group * GROUP_DIM
        own = values[:, start:start + GROUP_DIM]
        level = group % 4
        if level < 3:
            half_width = windows[level] // 2
            low = jnp.maximum(positions - half_width, begin)
            high = jnp.minimum(positions + half_width, finish)
            window_sum = prefix[high][:, start:start + GROUP_DIM] - prefix[low][:, start:start + GROUP_DIM]
            window_mean = window_sum / (high - low).astype(jnp.float32)[:, None]
        else:
            doc_sums = jax.ops.segment_sum(own, documents, num_segments=DOCS)
            window_mean = doc_sums[documents] / doc_count_f[documents][:, None]
        pool_diff = (window_mean - own).astype(jnp.bfloat16)
        pieces.append(jnp.dot(pool_diff, group_weights[group], preferred_element_type=jnp.float32))
    pooled = (jnp.concatenate(pieces, axis=1) * pool_gain.astype(jnp.float32)).astype(jnp.bfloat16)
    mixed = jnp.dot(pooled, output_weight, preferred_element_type=jnp.float32)
    stream = (residual.astype(jnp.float32) + rms_scale(mixed, mixer_gain)).astype(jnp.bfloat16)
    stream_f = lax.optimization_barrier(stream).astype(jnp.float32)
    normed = rms_scale(stream_f, routed_gain).astype(jnp.bfloat16)
    group_ids = chosen_group[:, 0]
    picked = (chosen_experts[:, :, None] == jnp.arange(EPG, dtype=jnp.int32)[None, None, :]).astype(jnp.float32)
    shares = lax.optimization_barrier(jnp.sum(expert_share.astype(jnp.float32)[:, :, None] * picked, axis=1))
    order = jnp.argsort(group_ids, stable=True).astype(jnp.int32)
    group_count = jax.ops.segment_sum(jnp.ones((TOKENS,), jnp.int32), group_ids, num_segments=GROUPS)
    padded_count = (group_count + row_block - 1) // row_block * row_block
    pad_end = jnp.cumsum(padded_count)
    pad_begin = pad_end - padded_count
    group_begin = jnp.cumsum(group_count) - group_count
    sorted_group = group_ids[order]
    dest = (pad_begin[sorted_group] + positions - group_begin[sorted_group]).astype(jnp.int32)
    block_total = (TOKENS + GROUPS * (row_block - 1)) // row_block + 1
    row_token = jnp.zeros((block_total * row_block,), jnp.int32).at[dest].set(order)
    row_live = jnp.zeros((block_total * row_block,), jnp.float32).at[dest].set(1.0)
    block_group = jnp.clip(jnp.searchsorted(pad_end, jnp.arange(block_total, dtype=jnp.int32) * row_block, side='right'), 0, GROUPS - 1).astype(jnp.int32)
    block_in = normed[row_token].reshape(block_total, row_block, D)
    block_share = (shares[row_token] * row_live[:, None]).reshape(block_total, row_block, EPG)

    def serve(item):
        return expert_rows(item[0], item[1], item[2], expert_gate, expert_up, expert_down)
    results = lax.map(serve, (block_in, block_share, block_group)).reshape(block_total * row_block, D)
    token_slot = jnp.zeros((TOKENS,), jnp.int32).at[order].set(dest)
    expert_out = results[token_slot]
    return (stream_f + rms_scale(expert_out.astype(jnp.float32), final_gain)).astype(jnp.bfloat16)
```

```python
import functools

import jax
import jax.numpy as jnp
from jax import lax
from jax.experimental import pallas as pl
from jax.experimental.pallas import tpu as pltpu
from jax.sharding import PartitionSpec as P

EPSILON = 1e-06


PHASES = 4
EARLY = 2
SEND_ORDER = (3, 0, 2, 1)
SERVE_ORDER = (3, 0, 2, 1)
LANES = 128


def greet():
    barrier = pltpu.get_barrier_semaphore()
    count = lax.axis_size("sp")
    me = lax.axis_index("sp")

    def signal(step, carry):
        pl.semaphore_signal(barrier, inc=1, device_id={"sp": lax.rem(me + step, count)})
        return carry

    lax.fori_loop(1, count, signal, 0)
    pl.semaphore_signal(barrier, inc=1, device_id={"tp": 1 - lax.axis_index("tp")})


def in_order(turn, order):
    phase = order[-1]
    for index in range(len(order) - 2, -1, -1):
        phase = jnp.where(turn == index, order[index], phase)
    return phase


def settle(ref, sem):
    pltpu.make_async_copy(ref, ref, sem).wait()


def other_plane(plane, phase):
    turn = PHASES - 1 - phase
    high = lax.rem(plane // 2 + turn // 2, 2)
    low = lax.rem(plane + turn, 2)
    return high * 2 + low


def mixer_stage(
    count,
    docs,
    me,
    tp_rank,
    pool_ref,
    docs_ref,
    weights_ref,
    pool_gain_ref,
    padded,
    edge_docs,
    table,
    tables,
    pooled,
    edge_send,
    edge_recv,
    table_send,
    table_recv,
    spread,
):
    length, part = pool_ref.shape
    reach = length // 2
    barrier = pltpu.get_barrier_semaphore()
    own_rows = pltpu.make_async_copy(pool_ref, padded.at[pl.ds(reach, length)], edge_recv.at[6])
    own_rows.start()
    own_docs = jnp.concatenate([docs_ref[0], docs_ref[1]], axis=1).astype(jnp.float32)
    group_dim = weights_ref.shape[1]
    low, high = slice(0, LANES), slice(part - LANES, part)
    hot = (
        lax.broadcasted_iota(jnp.int32, (docs, length), 0).astype(jnp.float32) == own_docs
    ).astype(jnp.float32)
    sums = jnp.dot(
        hot.astype(jnp.bfloat16), pool_ref[:, high], preferred_element_type=jnp.float32
    )
    global_lane = lax.broadcasted_iota(jnp.int32, (docs, LANES), 1) >= LANES - group_dim
    table[...] = jnp.where(global_lane, sums, jnp.sum(hot, axis=1, keepdims=True))
    local_copy = pltpu.make_async_copy(table, tables.at[me], table_recv.at[me])
    local_copy.start()
    pl.semaphore_wait(barrier, count)
    right, left = lax.rem(me + 1, count), lax.rem(me + count - 1, count)
    copies = []
    for side, target in enumerate((right, left)):
        for nth, (columns, deep) in enumerate(((low, reach // 2), (high, reach))):
            start = (length - deep) if side == 0 else 0
            into = (reach - deep) if side == 0 else (reach + length)
            copies.append(
                pltpu.make_async_remote_copy(
                    pool_ref.at[pl.ds(start, deep), columns],
                    padded.at[pl.ds(into, deep), columns],
                    edge_send.at[3 * side + nth],
                    edge_recv.at[3 * side + nth],
                    device_id={"sp": target},
                )
            )
        copies.append(
            pltpu.make_async_remote_copy(
                docs_ref.at[1 - side],
                edge_docs.at[side],
                edge_send.at[3 * side + 2],
                edge_recv.at[3 * side + 2],
                device_id={"sp": target},
            )
        )

    def table_copy(step):
        return pltpu.make_async_remote_copy(
            table,
            tables.at[me],
            table_send.at[step],
            table_recv.at[me],
            device_id={"sp": lax.rem(me + step, count)},
        )

    for copy in copies:
        copy.start()

    def start_table(step, carry):
        table_copy(step).start()
        return carry

    lax.fori_loop(1, count, start_table, 0)
    spread()

    local_groups = part // weights_ref.shape[1]
    bands = []
    for group in range(local_groups):
        own = weights_ref[tp_rank * local_groups + group]
        pieces = [jnp.zeros_like(own)] * local_groups
        pieces[group] = own
        bands.append(jnp.concatenate(pieces, axis=1))
    block_weight = jnp.concatenate(bands, axis=0)
    all_gain = pool_gain_ref[...].astype(jnp.float32).reshape(1, -1)
    gain = all_gain[:, :part]
    for other in range(1, all_gain.shape[1] // part):
        rest = all_gain[:, other * part : (other + 1) * part]
        gain = jnp.where(tp_rank == other, rest, gain)
    own_column = jnp.transpose(jnp.broadcast_to(own_docs, (LANES, length)))[:, :1]
    block = length // 4
    lane_group = lax.broadcasted_iota(jnp.int32, (block, LANES), 1) // group_dim
    first_half = lane_group == 0
    own_rows.wait()
    for copy in copies:
        copy.wait()
    before = jnp.where(me == 0, -1.0, edge_docs[0].astype(jnp.float32))
    after = jnp.where(me == count - 1, -1.0, edge_docs[1].astype(jnp.float32))
    all_docs = jnp.concatenate([before, own_docs, after], axis=1)

    def end_table(step, carry):
        settle(tables.at[step], table_recv.at[step])
        return carry

    lax.fori_loop(0, count, end_table, 0)
    totals = jnp.sum(tables[...], axis=0)
    doc_means = totals / totals[:, :1]
    for index in range(length // block):
        rows = slice(index * block, (index + 1) * block)
        column = own_column[rows]

        def window_mean(level, columns):
            half_width = length * (1 << level) // 8
            span = block + 2 * half_width
            start = reach + index * block - half_width
            offsets = (
                lax.broadcasted_iota(jnp.int32, (block, span), 1)
                - half_width
                - lax.broadcasted_iota(jnp.int32, (block, span), 0)
            )
            reached = slice(start, start + span)
            inside = (
                (all_docs[:, reached] == column)
                & (offsets >= -half_width)
                & (offsets < half_width)
            )
            mask = jnp.where(inside, 1.0, 0.0)
            sums = jnp.dot(
                mask.astype(jnp.bfloat16),
                padded[reached, columns],
                preferred_element_type=jnp.float32,
            )
            return sums / jnp.sum(mask, axis=1, keepdims=True)

        doc_mean = jnp.zeros((block, LANES), jnp.float32)
        for doc in range(docs):
            doc_mean = jnp.where(column == doc, doc_means[doc : doc + 1], doc_mean)
        mean = jnp.concatenate(
            [
                jnp.where(first_half, window_mean(0, low), window_mean(1, low)),
                jnp.where(first_half, window_mean(2, high), doc_mean),
            ],
            axis=1,
        )
        difference = (mean - pool_ref[rows].astype(jnp.float32)).astype(jnp.bfloat16)
        pooled[rows] = (
            jnp.dot(difference, block_weight, preferred_element_type=jnp.float32) * gain
        ).astype(jnp.bfloat16)

    def sent_table(step, carry):
        table_copy(step).wait_send()
        return carry

    lax.fori_loop(1, count, sent_table, 0)


def route(group_ref, experts_ref, share_ref, cap, slots, place, pick, share_send):
    rows = group_ref.shape[1]
    ids = group_ref[...]
    names = lax.broadcasted_iota(jnp.int32, (LANES, rows), 0)
    member = (ids == names).astype(jnp.float32)
    earlier = (
        lax.broadcasted_iota(jnp.int32, (rows, rows), 0)
        < lax.broadcasted_iota(jnp.int32, (rows, rows), 1)
    ).astype(jnp.float32)
    ahead = jnp.dot(
        member.astype(jnp.bfloat16),
        earlier.astype(jnp.bfloat16),
        preferred_element_type=jnp.float32,
    )
    rank = jnp.sum(ahead * member, axis=0, keepdims=True)
    slot = ids.astype(jnp.float32) * cap + rank
    chosen = (
        slot == lax.broadcasted_iota(jnp.int32, (slots, rows), 0).astype(jnp.float32)
    ).astype(jnp.float32)
    pick[...] = jnp.transpose(chosen).astype(jnp.bfloat16)
    place[...] = chosen.astype(jnp.bfloat16)
    spot = lax.broadcasted_iota(jnp.int32, (LANES, rows), 0)
    named = spot // cap
    total = jnp.zeros((LANES, rows), jnp.float32)
    for nth in range(experts_ref.shape[0]):
        here = experts_ref[nth : nth + 1] == named
        total = total + jnp.where(here, share_ref[nth : nth + 1].astype(jnp.float32), 0.0)
    total = jnp.where(rank == lax.rem(spot, cap).astype(jnp.float32), total, 0.0)
    sent = lax.dot_general(
        member.astype(jnp.bfloat16),
        total.astype(jnp.bfloat16),
        (((1,), (1,)), ((), ())),
        preferred_element_type=jnp.float32,
    )
    for dest in range(slots // cap):
        share_send[dest] = sent[dest : dest + 1]


def scaled(values, gain):
    return values * lax.rsqrt(jnp.mean(values * values, axis=-1, keepdims=True) + EPSILON) * gain


def layer_kernel(
    count,
    docs,
    pool_ref,
    docs_ref,
    residual_hbm,
    weights_ref,
    pool_gain_ref,
    output_hbm,
    mixer_gain_ref,
    routed_gain_ref,
    final_gain_ref,
    group_ref,
    experts_ref,
    share_ref,
    gate_hbm,
    up_hbm,
    down_hbm,
    out_ref,
    padded,
    edge_docs,
    table,
    tables,
    pooled,
    swapped,
    output_weight,
    residual,
    mixed,
    stream,
    wide,
    place,
    pick,
    share_send,
    arrived_share,
    early_send,
    early_recv,
    pooled_send,
    pooled_recv,
    far_mixed,
    send_ref,
    fetched,
    arrived,
    gates,
    ups,
    downs,
    hidden,
    kept,
    outgoing,
    incoming,
    result,
    edge_send,
    edge_recv,
    table_send,
    table_recv,
    swap_sem,
    spread_send,
    spread_recv,
    weight_sem,
    send_sem,
    recv_sem,
    forward_send,
    forward_recv,
    part_send,
    part_recv,
    back_send,
    back_recv,
    first_send,
    first_recv,
    second_send,
    second_recv,
):
    me, tp_rank = lax.axis_index("sp"), lax.axis_index("tp")
    per = count // PHASES
    plane, spot_of = me // per, lax.rem(me, per)
    rows, width = out_ref.shape
    slots = send_ref.shape[0]
    cap = slots // count
    experts, _, units = gates.shape
    half = per * cap
    part = pool_ref.shape[1]
    greet()

    def block(index):
        return pl.ds(pl.multiple_of(index * cap, cap), cap)

    def target(step):
        phase = step // per
        spot = lax.rem(step + spot_of, per)
        return phase, spot, other_plane(plane, phase) * per + spot

    residual_load = pltpu.make_async_copy(residual_hbm, residual, weight_sem.at[4])
    output_load = pltpu.make_async_copy(output_hbm, output_weight, weight_sem.at[3])
    loads = [
        pltpu.make_async_copy(gate_hbm, gates, weight_sem.at[0]),
        pltpu.make_async_copy(up_hbm, ups, weight_sem.at[1]),
        pltpu.make_async_copy(down_hbm, downs, weight_sem.at[2]),
    ]
    for load in [residual_load, output_load] + loads:
        load.start()
    route(group_ref, experts_ref, share_ref, cap, slots, place, pick, share_send)
    tile = width // 4
    tiles = [slice(index * tile, (index + 1) * tile) for index in range(4)]

    def far_dest(step):
        return other_plane(plane, 0) * per + lax.rem(step + spot_of, per)

    far_place = jnp.concatenate([place[block(far_dest(step))] for step in range(EARLY)], axis=0)
    residual_load.wait()
    for columns in tiles:
        early_send[:, columns] = jnp.dot(
            far_place, residual[:, columns], preferred_element_type=jnp.float32
        ).astype(jnp.bfloat16)

    def far_copies(step):
        here = pl.ds(step * cap, cap)
        return [
            pltpu.make_async_remote_copy(
                source.at[here],
                into.at[here],
                send.at[step],
                recv.at[step],
                device_id={"sp": far_dest(step)},
            )
            for source, into, send, recv in (
                (early_send, early_recv, first_send, first_recv),
                (pooled_send, pooled_recv, second_send, second_recv),
            )
        ]

    far = [far_copies(step) for step in range(EARLY)]

    def share_copy(step):
        phase, _, dest = target(step)
        return dest, pltpu.make_async_remote_copy(
            share_send.at[dest],
            arrived_share.at[phase, 0, spot_of],
            spread_send.at[step],
            spread_recv.at[phase * per + spot_of],
            device_id={"sp": dest},
        )

    def spread():
        pltpu.make_async_copy(
            share_send.at[me],
            arrived_share.at[PHASES - 1, 0, spot_of],
            spread_recv.at[(PHASES - 1) * per + spot_of],
        ).start()

        def start_share(step, carry):
            dest, copy = share_copy(step)

            @pl.when(dest != me)
            def _():
                copy.start()

            return carry

        lax.fori_loop(0, count, start_share, 0)
        for first, _ in far:
            first.start()

    mixer_stage(
        count,
        docs,
        me,
        tp_rank,
        pool_ref,
        docs_ref,
        weights_ref,
        pool_gain_ref,
        padded,
        edge_docs,
        table,
        tables,
        pooled,
        edge_send,
        edge_recv,
        table_send,
        table_recv,
        spread,
    )
    trade = pltpu.make_async_remote_copy(
        pooled.at[pl.ds(pl.multiple_of((1 - tp_rank) * rows, rows), rows)],
        swapped,
        swap_sem.at[0],
        swap_sem.at[1],
        device_id={"tp": 1 - tp_rank},
    )
    trade.start()
    output_load.wait()
    own_part = pooled[pl.ds(pl.multiple_of(tp_rank * rows, rows), rows)]
    own_from = pl.ds(pl.multiple_of(tp_rank * part, part), part)
    peer_from = pl.ds(pl.multiple_of((1 - tp_rank) * part, part), part)
    pooled_send[:, own_from] = jnp.dot(
        far_place, own_part, preferred_element_type=jnp.float32
    ).astype(jnp.bfloat16)
    for columns in tiles:
        mixed[:, columns] = jnp.dot(
            own_part, output_weight[own_from, columns], preferred_element_type=jnp.float32
        )
    trade.wait()
    pooled_send[:, peer_from] = jnp.dot(
        far_place, swapped[...], preferred_element_type=jnp.float32
    ).astype(jnp.bfloat16)
    for _, second in far:
        second.start()
    for columns in tiles:
        mixed[:, columns] += jnp.dot(
            swapped[...], output_weight[peer_from, columns], preferred_element_type=jnp.float32
        )
    mixer_gain = mixer_gain_ref[...].astype(jnp.float32).reshape(1, -1)
    routed_gain = routed_gain_ref[...].astype(jnp.float32).reshape(1, -1)
    final_gain = final_gain_ref[...].astype(jnp.float32).reshape(1, -1)
    chunk = 32

    def normalise(index, carry):
        here = pl.ds(pl.multiple_of(index * chunk, chunk), chunk)
        value = (
            residual[here].astype(jnp.float32) + scaled(mixed[here], mixer_gain)
        ).astype(jnp.bfloat16)
        stream[here] = value
        wide[here] = scaled(value.astype(jnp.float32), routed_gain).astype(jnp.bfloat16)
        return carry

    lax.fori_loop(0, rows // chunk, normalise, 0)
    def dispatch(step):
        phase = step // per
        spot = lax.rem(step + spot_of, per)
        dest = other_plane(plane, phase) * per + spot
        return dest, pltpu.make_async_remote_copy(
            send_ref.at[block(dest)],
            arrived.at[phase, block(spot_of)],
            send_sem.at[step],
            recv_sem.at[phase * per + spot_of],
            device_id={"sp": dest},
        )

    own_in = pltpu.make_async_copy(
        send_ref.at[block(me)],
        arrived.at[PHASES - 1, block(spot_of)],
        recv_sem.at[(PHASES - 1) * per + spot_of],
    )

    def start_dispatch(step, carry):
        dest, copy = dispatch(step)

        @pl.when(dest != me)
        def _():
            copy.start()

        return carry

    for phase in SEND_ORDER:
        there = pl.ds(pl.multiple_of(other_plane(plane, phase) * half, half), half)
        for columns in tiles:
            send_ref[there, columns] = jnp.dot(
                place[there], wide[:, columns], preferred_element_type=jnp.float32
            ).astype(jnp.bfloat16)
        begin = EARLY if phase == 0 else phase * per
        lax.fori_loop(begin, (phase + 1) * per, start_dispatch, 0)
        if phase == PHASES - 1:
            own_in.start()

    def end_share(step, carry):
        settle(
            arrived_share.at[step // per, 0, lax.rem(step, per)], spread_recv.at[step]
        )
        return carry

    lax.fori_loop(0, count, end_share, 0)
    share_forward = pltpu.make_async_remote_copy(
        arrived_share.at[:, 0],
        arrived_share.at[:, 1],
        swap_sem.at[2],
        swap_sem.at[3],
        device_id={"tp": 1 - tp_rank},
    )
    share_forward.start()
    for load in loads:
        load.wait()
    share_forward.wait()

    def back(step):
        phase = step // per
        spot = lax.rem(step + spot_of, per)
        dest = other_plane(plane, phase) * per + spot
        return dest, spot, pltpu.make_async_remote_copy(
            result.at[phase, block(spot)],
            fetched.at[block(me)],
            back_send.at[step],
            back_recv.at[me],
            device_id={"sp": dest},
        )

    own_back = pltpu.make_async_copy(
        result.at[PHASES - 1, block(spot_of)], fetched.at[block(me)], back_recv.at[me]
    )

    def meet_far():
        for step in range(EARLY):
            for copy in far[step]:
                copy.wait_recv()
        for columns in tiles:
            far_mixed[:, columns] = jnp.dot(
                pooled_recv[...], output_weight[:, columns], preferred_element_type=jnp.float32
            )
        for step in range(EARLY):
            here = pl.ds(step * cap, cap)
            value = (
                early_recv[here].astype(jnp.float32) + scaled(far_mixed[here], mixer_gain)
            ).astype(jnp.bfloat16)
            arrived[0, block(lax.rem(spot_of + per - step, per))] = scaled(
                value.astype(jnp.float32), routed_gain
            ).astype(jnp.bfloat16)

    def start_back(step, carry):
        dest, _, copy = back(step)

        @pl.when(dest != me)
        def _():
            copy.start()

        return carry

    def return_phase(phase):
        lax.fori_loop(phase * per, (phase + 1) * per, start_back, 0)

    def sent_near(step, carry):
        dispatch(step)[1].wait_send()
        return carry

    def serve(turn, carry):
        phase = in_order(turn, SERVE_ORDER)
        pieces = [arrived_share[phase, core, spot] for core in range(2) for spot in range(per)]
        pieces.append(jnp.zeros((LANES - 2 * per, LANES), jnp.float32))
        turned = jnp.transpose(jnp.concatenate(pieces, axis=0))

        def land(step, inner):
            spot = lax.rem(spot_of + per - step, per)
            settle(arrived.at[phase, block(spot)], recv_sem.at[phase * per + spot])
            return inner

        lax.fori_loop(jnp.where(phase == 0, EARLY, 0), per, land, 0)

        @pl.when(phase == 0)
        def _():
            meet_far()

        forward = pltpu.make_async_remote_copy(
            arrived.at[phase, pl.ds(0, half)],
            arrived.at[phase, pl.ds(half, half)],
            forward_send.at[phase],
            forward_recv.at[phase],
            device_id={"tp": 1 - tp_rank},
        )
        forward.start()
        forward.wait()
        for expert in range(experts):
            given = arrived[phase]
            gate = jnp.dot(given, gates[expert], preferred_element_type=jnp.float32)
            upper = jnp.dot(given, ups[expert], preferred_element_type=jnp.float32)
            silu = gate / (1.0 + jnp.exp(-gate))
            span = slice(expert * cap, (expert + 1) * cap)
            share = jnp.concatenate(
                [turned[span, column : column + 1] for column in range(2 * per)], axis=0
            )
            weighted = silu * upper * share
            hidden[:, expert * units : (expert + 1) * units] = weighted.astype(jnp.bfloat16)
        for columns in tiles:
            product = jnp.dot(hidden[...], downs[:, columns], preferred_element_type=jnp.float32)
            kept[:, columns] = product[:half]
            outgoing[phase, :, columns] = product[half:].astype(jnp.bfloat16)
        swap = pltpu.make_async_remote_copy(
            outgoing.at[phase],
            incoming.at[phase],
            part_send.at[phase],
            part_recv.at[phase],
            device_id={"tp": 1 - tp_rank},
        )
        swap.start()
        swap.wait()
        result[phase] = (kept[...] + incoming[phase].astype(jnp.float32)).astype(jnp.bfloat16)

        @pl.when(phase == 3)
        def _():
            return_phase(3)

        @pl.when(phase == 2)
        def _():
            lax.fori_loop(per, 2 * per, sent_near, 0)
            return_phase(0)
            return_phase(2)

        @pl.when(phase == 1)
        def _():
            return_phase(1)

        return carry

    lax.fori_loop(0, PHASES, serve, 0)
    own_back.start()

    def finish(step, carry):
        settle(fetched.at[block(step)], back_recv.at[step])
        dest, copy = dispatch(step)
        _, _, home = back(step)
        _, spread_out = share_copy(step)

        @pl.when((dest != me) & (step >= EARLY) & (step // per != 1))
        def _():
            copy.wait_send()

        @pl.when(dest != me)
        def _():
            home.wait_send()
            spread_out.wait_send()

        return carry

    for first, second in far:
        first.wait_send()
        second.wait_send()
    lax.fori_loop(0, count, finish, 0)
    for columns in tiles:
        mixed[:, columns] = jnp.dot(
            pick[...], fetched[:, columns], preferred_element_type=jnp.float32
        )

    def update(index, carry):
        here = pl.ds(pl.multiple_of(index * chunk, chunk), chunk)
        out_ref[here] = (
            stream[here].astype(jnp.float32) + scaled(mixed[here], final_gain)
        ).astype(jnp.bfloat16)
        return carry

    lax.fori_loop(0, rows // chunk, update, 0)


def local(
    pool_input,
    documents,
    residual,
    group_weights,
    pool_gain,
    output_weight,
    mixer_gain,
    routed_gain,
    final_gain,
    chosen_group,
    chosen_experts,
    expert_share,
    expert_gate,
    expert_up,
    expert_down,
):
    count = lax.axis_size("sp")
    docs = count // 4
    rows, width = residual.shape
    length, part = pool_input.shape
    reach = length // 2
    cap = length // count
    slots = count * cap
    per = count // PHASES
    half = per * cap
    down = expert_down.reshape(-1, width)
    bf16, f32 = jnp.bfloat16, jnp.float32
    dma, vmem = pltpu.SemaphoreType.DMA, pltpu.VMEM
    whole = pl.BlockSpec(memory_space=pltpu.VMEM)
    outside = pl.BlockSpec(memory_space=pl.ANY)
    return pl.pallas_call(
        functools.partial(layer_kernel, count, docs),
        out_shape=jax.ShapeDtypeStruct((rows, width), bf16),
        in_specs=[whole, whole, outside, whole, whole, outside]
        + [whole] * 6
        + [outside] * 3,
        out_specs=whole,
        scratch_shapes=[
            vmem((length + 2 * reach, part), bf16),
            vmem((2, 1, reach), documents.dtype),
            vmem((docs, LANES), f32),
            vmem((count, docs, LANES), f32),
            vmem((length, part), bf16),
            vmem((rows, part), bf16),
            vmem(output_weight.shape, bf16),
            vmem((rows, width), bf16),
            vmem((rows, width), f32),
            vmem((rows, width), bf16),
            vmem((rows, width), bf16),
            vmem((slots, rows), bf16),
            vmem((rows, slots), bf16),
            vmem((count, 1, LANES), f32),
            vmem((PHASES, 2, per, 1, LANES), f32),
            vmem((EARLY * cap, width), bf16),
            vmem((EARLY * cap, width), bf16),
            vmem((EARLY * cap, 2 * part), bf16),
            vmem((EARLY * cap, 2 * part), bf16),
            vmem((EARLY * cap, width), f32),
            vmem((slots, width), bf16),
            vmem((slots, width), bf16),
            vmem((PHASES, 2 * half, width), bf16),
            vmem(expert_gate.shape, bf16),
            vmem(expert_up.shape, bf16),
            vmem(down.shape, bf16),
            vmem((2 * half, down.shape[0]), bf16),
            vmem((half, width), f32),
            vmem((PHASES, half, width), bf16),
            vmem((PHASES, half, width), bf16),
            vmem((PHASES, half, width), bf16),
            dma((6,)),
            dma((7,)),
            dma((count,)),
            dma((count,)),
            dma((4,)),
            dma((count,)),
            dma((count,)),
            dma((5,)),
            dma((count,)),
            dma((count,)),
            dma((PHASES,)),
            dma((PHASES,)),
            dma((PHASES,)),
            dma((PHASES,)),
            dma((count,)),
            dma((count,)),
            dma((EARLY,)),
            dma((EARLY,)),
            dma((EARLY,)),
            dma((EARLY,)),
        ],
        compiler_params=pltpu.CompilerParams(
            collective_id=0, has_side_effects=True, vmem_limit_bytes=60 * 1024 * 1024
        ),
    )(
        pool_input,
        documents.reshape(2, 1, reach),
        residual,
        group_weights,
        pool_gain,
        output_weight,
        mixer_gain,
        routed_gain,
        final_gain,
        chosen_group.T,
        chosen_experts.T,
        expert_share.T,
        expert_gate,
        expert_up,
        down,
    )


def solution(mesh):
    placed = (
        P("sp", "tp"),
        P("sp"),
        P(("sp", "tp"), None),
        P(),
        P(),
        P(),
        P(),
        P(),
        P(),
        P(("sp", "tp"), None),
        P(("sp", "tp"), None),
        P(("sp", "tp"), None),
        P("sp", None, "tp"),
        P("sp", None, "tp"),
        P("sp", "tp", None),
    )
    return jax.shard_map(
        local, mesh=mesh, in_specs=placed, out_specs=P(("sp", "tp"), None), check_vma=False
    )
```

```python
import functools

import jax
import jax.numpy as jnp
from jax import lax
from jax.experimental import pallas as pl
from jax.experimental.pallas import tpu as pltpu
from jax.sharding import PartitionSpec as P

EPSILON = 1e-06


PHASES = 4
EARLY = 3
EAGER = 1
HOLDTURN = 1
FINISH_ORDER = (3, 2, 0, 1)
SEND_ORDER = (3, 0, 2, 1)
SERVE_ORDER = (3, 0, 2, 1)
LANES = 128


def greet():
    barrier = pltpu.get_barrier_semaphore()
    count = lax.axis_size("sp")
    me = lax.axis_index("sp")

    def signal(step, carry):
        pl.semaphore_signal(barrier, inc=1, device_id={"sp": lax.rem(me + step, count)})
        return carry

    lax.fori_loop(1, count, signal, 0)
    pl.semaphore_signal(barrier, inc=1, device_id={"tp": 1 - lax.axis_index("tp")})


def in_order(turn, order):
    phase = order[-1]
    for index in range(len(order) - 2, -1, -1):
        phase = jnp.where(turn == index, order[index], phase)
    return phase


def settle(ref, sem):
    pltpu.make_async_copy(ref, ref, sem).wait()


def other_plane(plane, phase):
    turn = PHASES - 1 - phase
    high = lax.rem(plane // 2 + turn // 2, 2)
    low = lax.rem(plane + turn, 2)
    return high * 2 + low


def mixer_stage(
    count,
    docs,
    me,
    tp_rank,
    pool_ref,
    docs_ref,
    weights_ref,
    pool_gain_ref,
    padded,
    packed,
    unpacked,
    edge_docs,
    table,
    tables,
    pooled,
    edge_send,
    edge_recv,
    table_send,
    table_recv,
    spread,
):
    length, part = pool_ref.shape
    reach = length // 2
    barrier = pltpu.get_barrier_semaphore()
    own_rows = pltpu.make_async_copy(pool_ref, padded.at[pl.ds(reach, length)], edge_recv.at[6])
    own_rows.start()
    own_docs = jnp.concatenate([docs_ref[0], docs_ref[1]], axis=1).astype(jnp.float32)
    group_dim = weights_ref.shape[1]
    low, high = slice(0, LANES), slice(part - LANES, part)
    hot = (
        lax.broadcasted_iota(jnp.int32, (docs, length), 0).astype(jnp.float32) == own_docs
    ).astype(jnp.float32)
    sums = jnp.dot(
        hot.astype(jnp.bfloat16), pool_ref[:, high], preferred_element_type=jnp.float32
    )
    global_lane = lax.broadcasted_iota(jnp.int32, (docs, LANES), 1) >= LANES - group_dim
    table[...] = jnp.where(global_lane, sums, jnp.sum(hot, axis=1, keepdims=True))
    deep = reach // 2
    front = lax.broadcasted_iota(jnp.int32, (deep, LANES), 1) < group_dim
    for side, start in enumerate((length - reach, 0)):
        first = pool_ref[pl.ds(start, deep), high].astype(jnp.float32)
        second = pool_ref[pl.ds(start + deep, deep), high].astype(jnp.float32)
        packed[side] = jnp.where(
            front, first, pltpu.roll(second, group_dim, 1)
        ).astype(jnp.bfloat16)
    local_copy = pltpu.make_async_copy(table, tables.at[me], table_recv.at[0])
    local_copy.start()
    pl.semaphore_wait(barrier, count)
    right, left = lax.rem(me + 1, count), lax.rem(me + count - 1, count)
    copies = []
    for side, target in enumerate((right, left)):
        start = length - deep if side == 0 else 0
        into = reach - deep if side == 0 else reach + length
        for nth, (source, place) in enumerate(
            (
                (
                    pool_ref.at[pl.ds(start, deep), low],
                    padded.at[pl.ds(into, deep), low],
                ),
                (packed.at[side], unpacked.at[side]),
                (docs_ref.at[1 - side], edge_docs.at[side]),
            )
        ):
            copies.append(
                pltpu.make_async_remote_copy(
                    source,
                    place,
                    edge_send.at[3 * side + nth],
                    edge_recv.at[3 * side + nth],
                    device_id={"sp": target},
                )
            )

    def table_copy(step):
        return pltpu.make_async_remote_copy(
            table,
            tables.at[me],
            table_send.at[0],
            table_recv.at[0],
            device_id={"sp": lax.rem(me + step, count)},
        )

    for copy in copies:
        copy.start()

    def start_table(step, carry):
        table_copy(step).start()
        return carry

    lax.fori_loop(1, count, start_table, 0)
    spread()

    local_groups = part // weights_ref.shape[1]
    bands = []
    for group in range(local_groups):
        own = weights_ref[tp_rank * local_groups + group]
        pieces = [jnp.zeros_like(own)] * local_groups
        pieces[group] = own
        bands.append(jnp.concatenate(pieces, axis=1))
    block_weight = jnp.concatenate(bands, axis=0)
    all_gain = pool_gain_ref[...].astype(jnp.float32).reshape(1, -1)
    gain = all_gain[:, :part]
    for other in range(1, all_gain.shape[1] // part):
        rest = all_gain[:, other * part : (other + 1) * part]
        gain = jnp.where(tp_rank == other, rest, gain)
    own_column = jnp.transpose(jnp.broadcast_to(own_docs, (LANES, length)))[:, :1]
    block = length // 4
    lane_group = lax.broadcasted_iota(jnp.int32, (block, LANES), 1) // group_dim
    first_half = lane_group == 0
    own_rows.wait()
    for copy in copies:
        copy.wait()
    for side, start in enumerate((0, reach + length)):
        both = unpacked[side]
        padded[pl.ds(start, deep), high] = both
        padded[pl.ds(start + deep, deep), high] = pltpu.roll(
            both.astype(jnp.float32), LANES - group_dim, 1
        ).astype(jnp.bfloat16)
    before = jnp.where(me == 0, -1.0, edge_docs[0].astype(jnp.float32))
    after = jnp.where(me == count - 1, -1.0, edge_docs[1].astype(jnp.float32))
    all_docs = jnp.concatenate([before, own_docs, after], axis=1)

    settle(tables, table_recv.at[0])
    totals = jnp.sum(tables[...], axis=0)
    doc_means = totals / totals[:, :1]
    for index in range(length // block):
        rows = slice(index * block, (index + 1) * block)
        column = own_column[rows]

        def window_mean(level, columns):
            half_width = length * (1 << level) // 8
            span = block + 2 * half_width
            start = reach + index * block - half_width
            offsets = (
                lax.broadcasted_iota(jnp.int32, (block, span), 1)
                - half_width
                - lax.broadcasted_iota(jnp.int32, (block, span), 0)
            )
            reached = slice(start, start + span)
            inside = (
                (all_docs[:, reached] == column)
                & (offsets >= -half_width)
                & (offsets < half_width)
            )
            mask = jnp.where(inside, 1.0, 0.0)
            sums = jnp.dot(
                mask.astype(jnp.bfloat16),
                padded[reached, columns],
                preferred_element_type=jnp.float32,
            )
            return sums / jnp.sum(mask, axis=1, keepdims=True)

        doc_mean = jnp.zeros((block, LANES), jnp.float32)
        for doc in range(docs):
            doc_mean = jnp.where(column == doc, doc_means[doc : doc + 1], doc_mean)
        mean = jnp.concatenate(
            [
                jnp.where(first_half, window_mean(0, low), window_mean(1, low)),
                jnp.where(first_half, window_mean(2, high), doc_mean),
            ],
            axis=1,
        )
        difference = (mean - pool_ref[rows].astype(jnp.float32)).astype(jnp.bfloat16)
        pooled[rows] = (
            jnp.dot(difference, block_weight, preferred_element_type=jnp.float32) * gain
        ).astype(jnp.bfloat16)

    settle(tables.at[pl.ds(0, count - 1)], table_send.at[0])


def route(group_ref, experts_ref, share_ref, cap, slots, place, pick, share_send):
    rows = group_ref.shape[1]
    ids = group_ref[...]
    names = lax.broadcasted_iota(jnp.int32, (LANES, rows), 0)
    member = (ids == names).astype(jnp.float32)
    earlier = (
        lax.broadcasted_iota(jnp.int32, (rows, rows), 0)
        < lax.broadcasted_iota(jnp.int32, (rows, rows), 1)
    ).astype(jnp.float32)
    ahead = jnp.dot(
        member.astype(jnp.bfloat16),
        earlier.astype(jnp.bfloat16),
        preferred_element_type=jnp.float32,
    )
    rank = jnp.sum(ahead * member, axis=0, keepdims=True)
    slot = ids.astype(jnp.float32) * cap + rank
    chosen = (
        slot == lax.broadcasted_iota(jnp.int32, (slots, rows), 0).astype(jnp.float32)
    ).astype(jnp.float32)
    pick[...] = jnp.transpose(chosen).astype(jnp.bfloat16)
    place[...] = chosen.astype(jnp.bfloat16)
    spot = lax.broadcasted_iota(jnp.int32, (LANES, rows), 0)
    named = spot // cap
    total = jnp.zeros((LANES, rows), jnp.float32)
    for nth in range(experts_ref.shape[0]):
        here = experts_ref[nth : nth + 1] == named
        total = total + jnp.where(here, share_ref[nth : nth + 1].astype(jnp.float32), 0.0)
    total = jnp.where(rank == lax.rem(spot, cap).astype(jnp.float32), total, 0.0)
    sent = lax.dot_general(
        member.astype(jnp.bfloat16),
        total.astype(jnp.bfloat16),
        (((1,), (1,)), ((), ())),
        preferred_element_type=jnp.float32,
    )
    for dest in range(slots // cap):
        share_send[dest] = sent[dest : dest + 1]


def scaled(values, gain):
    return values * lax.rsqrt(jnp.mean(values * values, axis=-1, keepdims=True) + EPSILON) * gain


def layer_kernel(
    count,
    docs,
    pool_ref,
    docs_ref,
    residual_hbm,
    weights_ref,
    pool_gain_ref,
    output_hbm,
    mixer_gain_ref,
    routed_gain_ref,
    final_gain_ref,
    group_ref,
    experts_ref,
    share_ref,
    gate_hbm,
    up_hbm,
    down_hbm,
    out_hbm,
    padded,
    packed,
    unpacked,
    edge_docs,
    table,
    tables,
    pooled,
    swapped,
    output_weight,
    residual,
    mixed,
    stream,
    wide,
    place,
    pick,
    share_send,
    arrived_share,
    early_send,
    early_recv,
    pooled_send,
    pooled_recv,
    far_mixed,
    send_ref,
    fetched,
    arrived,
    gates,
    ups,
    downs,
    hidden,
    kept,
    outgoing,
    incoming,
    result,
    slot_stream,
    final,
    edge_send,
    edge_recv,
    table_send,
    table_recv,
    swap_sem,
    spread_send,
    spread_recv,
    weight_sem,
    send_sem,
    recv_sem,
    forward_send,
    forward_recv,
    part_send,
    part_recv,
    back_send,
    back_recv,
    first_send,
    first_recv,
    second_send,
    second_recv,
    write_sem,
):
    me, tp_rank = lax.axis_index("sp"), lax.axis_index("tp")
    per = count // PHASES
    plane, spot_of = me // per, lax.rem(me, per)
    rows, width = out_hbm.shape
    slots = send_ref.shape[0]
    cap = slots // count
    experts, _, units = gates.shape
    half = per * cap
    part = pool_ref.shape[1]
    greet()

    def block(index):
        return pl.ds(pl.multiple_of(index * cap, cap), cap)

    def target(step):
        phase = step // per
        spot = lax.rem(step + spot_of, per)
        return phase, spot, other_plane(plane, phase) * per + spot

    residual_load = pltpu.make_async_copy(residual_hbm, residual, weight_sem.at[4])
    output_load = pltpu.make_async_copy(output_hbm, output_weight, weight_sem.at[3])
    loads = [
        pltpu.make_async_copy(gate_hbm, gates, weight_sem.at[0]),
        pltpu.make_async_copy(up_hbm, ups, weight_sem.at[1]),
        pltpu.make_async_copy(down_hbm, downs, weight_sem.at[2]),
    ]
    for load in [residual_load, output_load] + loads:
        load.start()
    route(group_ref, experts_ref, share_ref, cap, slots, place, pick, share_send)
    tile = width // 4
    tiles = [slice(index * tile, (index + 1) * tile) for index in range(4)]

    def far_dest(step):
        return other_plane(plane, 0) * per + lax.rem(step + spot_of, per)

    far_place = jnp.concatenate([place[block(far_dest(step))] for step in range(EARLY)], axis=0)
    residual_load.wait()
    for columns in tiles:
        early_send[:, columns] = jnp.dot(
            far_place, residual[:, columns], preferred_element_type=jnp.float32
        ).astype(jnp.bfloat16)

    def far_copies(step):
        here = pl.ds(step * cap, cap)
        return [
            pltpu.make_async_remote_copy(
                source.at[here],
                into.at[here],
                send.at[0],
                recv.at[0],
                device_id={"sp": far_dest(step)},
            )
            for source, into, send, recv in (
                (early_send, early_recv, first_send, first_recv),
                (pooled_send, pooled_recv, second_send, second_recv),
            )
        ]

    far = [far_copies(step) for step in range(EARLY)]

    def share_copy(step):
        phase, _, dest = target(step)
        return dest, pltpu.make_async_remote_copy(
            share_send.at[dest],
            arrived_share.at[phase, 0, spot_of],
            spread_send.at[0],
            spread_recv.at[0],
            device_id={"sp": dest},
        )

    def spread():
        pltpu.make_async_copy(
            share_send.at[me],
            arrived_share.at[PHASES - 1, 0, spot_of],
            spread_recv.at[0],
        ).start()

        def start_share(step, carry):
            dest, copy = share_copy(step)

            @pl.when(dest != me)
            def _():
                copy.start()

            return carry

        lax.fori_loop(0, count, start_share, 0)
        for first, _ in far:
            first.start()

    mixer_stage(
        count,
        docs,
        me,
        tp_rank,
        pool_ref,
        docs_ref,
        weights_ref,
        pool_gain_ref,
        padded,
        packed,
        unpacked,
        edge_docs,
        table,
        tables,
        pooled,
        edge_send,
        edge_recv,
        table_send,
        table_recv,
        spread,
    )
    trade = pltpu.make_async_remote_copy(
        pooled.at[pl.ds(pl.multiple_of((1 - tp_rank) * rows, rows), rows)],
        swapped,
        swap_sem.at[0],
        swap_sem.at[1],
        device_id={"tp": 1 - tp_rank},
    )
    trade.start()
    output_load.wait()
    own_part = pooled[pl.ds(pl.multiple_of(tp_rank * rows, rows), rows)]
    own_from = pl.ds(pl.multiple_of(tp_rank * part, part), part)
    peer_from = pl.ds(pl.multiple_of((1 - tp_rank) * part, part), part)
    pooled_send[:, own_from] = jnp.dot(
        far_place, own_part, preferred_element_type=jnp.float32
    ).astype(jnp.bfloat16)
    for columns in tiles:
        mixed[:, columns] = jnp.dot(
            own_part, output_weight[own_from, columns], preferred_element_type=jnp.float32
        )
    trade.wait()
    pooled_send[:, peer_from] = jnp.dot(
        far_place, swapped[...], preferred_element_type=jnp.float32
    ).astype(jnp.bfloat16)
    for _, second in far:
        second.start()
    for columns in tiles:
        mixed[:, columns] += jnp.dot(
            swapped[...], output_weight[peer_from, columns], preferred_element_type=jnp.float32
        )
    mixer_gain = mixer_gain_ref[...].astype(jnp.float32).reshape(1, -1)
    routed_gain = routed_gain_ref[...].astype(jnp.float32).reshape(1, -1)
    final_gain = final_gain_ref[...].astype(jnp.float32).reshape(1, -1)
    chunk = 32

    def normalise(index, carry):
        here = pl.ds(pl.multiple_of(index * chunk, chunk), chunk)
        value = (
            residual[here].astype(jnp.float32) + scaled(mixed[here], mixer_gain)
        ).astype(jnp.bfloat16)
        stream[here] = value
        wide[here] = scaled(value.astype(jnp.float32), routed_gain).astype(jnp.bfloat16)
        return carry

    lax.fori_loop(0, rows // chunk, normalise, 0)
    def dispatch(step):
        phase = step // per
        spot = lax.rem(step + spot_of, per)
        dest = other_plane(plane, phase) * per + spot
        return dest, pltpu.make_async_remote_copy(
            send_ref.at[block(dest)],
            arrived.at[phase, block(spot_of)],
            send_sem.at[phase],
            recv_sem.at[phase],
            device_id={"sp": dest},
        )

    own_in = pltpu.make_async_copy(
        send_ref.at[block(me)],
        arrived.at[PHASES - 1, block(spot_of)],
        recv_sem.at[PHASES - 1],
    )

    def start_dispatch(step, carry):
        dest, copy = dispatch(step)

        @pl.when(dest != me)
        def _():
            copy.start()

        return carry

    for phase in SEND_ORDER:
        there = pl.ds(pl.multiple_of(other_plane(plane, phase) * half, half), half)
        for columns in tiles:
            send_ref[there, columns] = jnp.dot(
                place[there], wide[:, columns], preferred_element_type=jnp.float32
            ).astype(jnp.bfloat16)
        begin = EARLY if phase == 0 else phase * per
        lax.fori_loop(begin, (phase + 1) * per, start_dispatch, 0)
        if phase == PHASES - 1:
            own_in.start()

    for phase in range(PHASES):
        there = pl.ds(phase * half, half)
        for columns in tiles:
            slot_stream[there, columns] = jnp.dot(
                place[there], stream[:, columns], preferred_element_type=jnp.float32
            ).astype(jnp.bfloat16)

    settle(arrived_share.at[:, 0], spread_recv.at[0])
    share_forward = pltpu.make_async_remote_copy(
        arrived_share.at[:, 0],
        arrived_share.at[:, 1],
        swap_sem.at[2],
        swap_sem.at[3],
        device_id={"tp": 1 - tp_rank},
    )
    share_forward.start()
    for load in loads:
        load.wait()
    share_forward.wait()

    def back(step):
        phase = step // per
        spot = lax.rem(step + spot_of, per)
        dest = other_plane(plane, phase) * per + spot
        return dest, spot, pltpu.make_async_remote_copy(
            result.at[phase, block(spot)],
            fetched.at[block(me)],
            back_send.at[0],
            back_recv.at[phase],
            device_id={"sp": dest},
        )

    own_back = pltpu.make_async_copy(
        result.at[PHASES - 1, block(spot_of)], fetched.at[block(me)], back_recv.at[PHASES - 1]
    )

    def meet_far():
        settle(early_recv, first_recv.at[0])
        settle(pooled_recv, second_recv.at[0])
        for columns in tiles:
            far_mixed[:, columns] = jnp.dot(
                pooled_recv[...], output_weight[:, columns], preferred_element_type=jnp.float32
            )
        for step in range(EARLY):
            here = pl.ds(step * cap, cap)
            value = (
                early_recv[here].astype(jnp.float32) + scaled(far_mixed[here], mixer_gain)
            ).astype(jnp.bfloat16)
            arrived[0, block(lax.rem(spot_of + per - step, per))] = scaled(
                value.astype(jnp.float32), routed_gain
            ).astype(jnp.bfloat16)

    def start_back(step, carry):
        dest, _, copy = back(step)

        @pl.when(dest != me)
        def _():
            copy.start()

        return carry

    def return_phase(phase):
        lax.fori_loop(phase * per, (phase + 1) * per, start_back, 0)

    def forward(phase):
        return pltpu.make_async_remote_copy(
            arrived.at[phase, pl.ds(0, half)],
            arrived.at[phase, pl.ds(half, half)],
            forward_send.at[phase],
            forward_recv.at[phase],
            device_id={"tp": 1 - tp_rank},
        )

    def land(phase):
        @pl.when(phase == 0)
        def _():
            if EARLY < per:
                settle(arrived.at[0, pl.ds(0, half - EARLY * cap)], recv_sem.at[0])
            meet_far()

        @pl.when(phase != 0)
        def _():
            settle(arrived.at[phase, pl.ds(0, half)], recv_sem.at[phase])

        forward(phase).start()

    def swap(phase, index):
        columns = tiles[index]
        return pltpu.make_async_remote_copy(
            outgoing.at[phase, :, columns],
            incoming.at[phase, :, columns],
            part_send.at[phase],
            part_recv.at[phase],
            device_id={"tp": 1 - tp_rank},
        )

    land(SERVE_ORDER[0])

    def serve(turn, carry):
        phase = in_order(turn, SERVE_ORDER)
        later = in_order(turn, SERVE_ORDER[1:] + (0,))
        pieces = [arrived_share[phase, core, spot] for core in range(2) for spot in range(per)]
        pieces.append(jnp.zeros((LANES - 2 * per, LANES), jnp.float32))
        turned = jnp.transpose(jnp.concatenate(pieces, axis=0))
        forward(phase).wait()

        @pl.when(turn == EAGER)
        def _():
            land(later)

        for expert in range(experts):
            given = arrived[phase]
            gate = jnp.dot(given, gates[expert], preferred_element_type=jnp.float32)
            upper = jnp.dot(given, ups[expert], preferred_element_type=jnp.float32)
            silu = gate / (1.0 + jnp.exp(-gate))
            span = slice(expert * cap, (expert + 1) * cap)
            share = jnp.concatenate(
                [turned[span, column : column + 1] for column in range(2 * per)], axis=0
            )
            weighted = silu * upper * share
            hidden[:, expert * units : (expert + 1) * units] = weighted.astype(jnp.bfloat16)
        for index, columns in enumerate(tiles):
            product = jnp.dot(hidden[...], downs[:, columns], preferred_element_type=jnp.float32)
            kept[:, columns] = product[:half]
            outgoing[phase, :, columns] = product[half:].astype(jnp.bfloat16)
            swap(phase, index).start()

        @pl.when((turn != EAGER) & (turn < PHASES - 1))
        def _():
            land(later)

        settle(outgoing.at[phase], part_send.at[phase])
        settle(incoming.at[phase], part_recv.at[phase])
        for columns in tiles:
            result[phase, :, columns] = (
                kept[:, columns] + incoming[phase, :, columns].astype(jnp.float32)
            ).astype(jnp.bfloat16)

        @pl.when(turn == HOLDTURN)
        def _():
            settle(send_ref.at[pl.ds(0, half)], send_sem.at[1])
            return_phase(0)

        @pl.when(phase != 0)
        def _():
            return_phase(phase)

        return carry

    lax.fori_loop(0, PHASES, serve, 0)
    own_back.start()

    for phase in FINISH_ORDER:
        origin = other_plane(plane, phase)

        def update(index, carry):
            here = pl.ds(pl.multiple_of(origin * half + index * chunk, chunk), chunk)
            slot_stream[here] = (
                slot_stream[here].astype(jnp.float32)
                + scaled(fetched[here].astype(jnp.float32), final_gain)
            ).astype(jnp.bfloat16)
            return carry

        settle(fetched.at[pl.ds(0, half)], back_recv.at[phase])
        lax.fori_loop(0, half // chunk, update, 0)
    writes = []
    for index, columns in enumerate(tiles):
        final[:, columns] = jnp.dot(
            pick[...], slot_stream[:, columns], preferred_element_type=jnp.float32
        ).astype(jnp.bfloat16)
        writes.append(
            pltpu.make_async_copy(
                final.at[:, columns], out_hbm.at[:, columns], write_sem.at[index]
            )
        )
        writes[-1].start()
    settle(early_send, first_send.at[0])
    settle(pooled_send, second_send.at[0])
    settle(share_send.at[pl.ds(0, count - 1)], spread_send.at[0])
    settle(fetched.at[pl.ds(0, (count - 1) * cap)], back_send.at[0])
    for phase, blocks in ((0, per - EARLY), (2, per), (3, per - 1)):
        settle(send_ref.at[pl.ds(0, blocks * cap)], send_sem.at[phase])
    for write in writes:
        write.wait()


def local(
    pool_input,
    documents,
    residual,
    group_weights,
    pool_gain,
    output_weight,
    mixer_gain,
    routed_gain,
    final_gain,
    chosen_group,
    chosen_experts,
    expert_share,
    expert_gate,
    expert_up,
    expert_down,
):
    count = lax.axis_size("sp")
    docs = count // 4
    rows, width = residual.shape
    length, part = pool_input.shape
    reach = length // 2
    cap = length // count
    slots = count * cap
    per = count // PHASES
    half = per * cap
    down = expert_down.reshape(-1, width)
    bf16, f32 = jnp.bfloat16, jnp.float32
    dma, vmem = pltpu.SemaphoreType.DMA, pltpu.VMEM
    whole = pl.BlockSpec(memory_space=pltpu.VMEM)
    outside = pl.BlockSpec(memory_space=pl.ANY)
    return pl.pallas_call(
        functools.partial(layer_kernel, count, docs),
        out_shape=jax.ShapeDtypeStruct((rows, width), bf16),
        in_specs=[whole, whole, outside, whole, whole, outside]
        + [whole] * 6
        + [outside] * 3,
        out_specs=outside,
        scratch_shapes=[
            vmem((length + 2 * reach, part), bf16),
            vmem((2, reach // 2, LANES), bf16),
            vmem((2, reach // 2, LANES), bf16),
            vmem((2, 1, reach), documents.dtype),
            vmem((docs, LANES), f32),
            vmem((count, docs, LANES), f32),
            vmem((length, part), bf16),
            vmem((rows, part), bf16),
            vmem(output_weight.shape, bf16),
            vmem((rows, width), bf16),
            vmem((rows, width), f32),
            vmem((rows, width), bf16),
            vmem((rows, width), bf16),
            vmem((slots, rows), bf16),
            vmem((rows, slots), bf16),
            vmem((count, 1, LANES), f32),
            vmem((PHASES, 2, per, 1, LANES), f32),
            vmem((EARLY * cap, width), bf16),
            vmem((EARLY * cap, width), bf16),
            vmem((EARLY * cap, 2 * part), bf16),
            vmem((EARLY * cap, 2 * part), bf16),
            vmem((EARLY * cap, width), f32),
            vmem((slots, width), bf16),
            vmem((slots, width), bf16),
            vmem((PHASES, 2 * half, width), bf16),
            vmem(expert_gate.shape, bf16),
            vmem(expert_up.shape, bf16),
            vmem(down.shape, bf16),
            vmem((2 * half, down.shape[0]), bf16),
            vmem((half, width), f32),
            vmem((PHASES, half, width), bf16),
            vmem((PHASES, half, width), bf16),
            vmem((PHASES, half, width), bf16),
            vmem((slots, width), bf16),
            vmem((rows, width), bf16),
            dma((6,)),
            dma((7,)),
            dma((1,)),
            dma((1,)),
            dma((4,)),
            dma((1,)),
            dma((1,)),
            dma((5,)),
            dma((PHASES,)),
            dma((PHASES,)),
            dma((PHASES,)),
            dma((PHASES,)),
            dma((PHASES,)),
            dma((PHASES,)),
            dma((1,)),
            dma((PHASES,)),
            dma((1,)),
            dma((1,)),
            dma((1,)),
            dma((1,)),
            dma((4,)),
        ],
        compiler_params=pltpu.CompilerParams(
            collective_id=0, has_side_effects=True, vmem_limit_bytes=60 * 1024 * 1024
        ),
    )(
        pool_input,
        documents.reshape(2, 1, reach),
        residual,
        group_weights,
        pool_gain,
        output_weight,
        mixer_gain,
        routed_gain,
        final_gain,
        chosen_group.T,
        chosen_experts.T,
        expert_share.T,
        expert_gate,
        expert_up,
        down,
    )


def solution(mesh):
    placed = (
        P("sp", "tp"),
        P("sp"),
        P(("sp", "tp"), None),
        P(),
        P(),
        P(),
        P(),
        P(),
        P(),
        P(("sp", "tp"), None),
        P(("sp", "tp"), None),
        P(("sp", "tp"), None),
        P("sp", None, "tp"),
        P("sp", None, "tp"),
        P("sp", "tp", None),
    )
    return jax.shard_map(
        local, mesh=mesh, in_specs=placed, out_specs=P(("sp", "tp"), None), check_vma=False
    )
```

```python
import functools

import jax
import jax.numpy as jnp
from jax import lax
from jax.experimental import pallas as pl
from jax.experimental.pallas import tpu as pltpu
from jax.sharding import PartitionSpec as P

EPSILON = 1e-06


PHASES = 4
EARLY = 3
EAGER = 1
HOLDTURN = 1
FINISH_ORDER = (3, 2, 0, 1)
SEND_ORDER = (3, 0, 2, 1)
SERVE_ORDER = (3, 0, 2, 1)
LANES = 128


def greet():
    barrier = pltpu.get_barrier_semaphore()
    count = lax.axis_size("sp")
    me = lax.axis_index("sp")

    def signal(step, carry):
        pl.semaphore_signal(barrier, inc=1, device_id={"sp": lax.rem(me + step, count)})
        return carry

    lax.fori_loop(1, count, signal, 0)
    pl.semaphore_signal(barrier, inc=1, device_id={"tp": 1 - lax.axis_index("tp")})


def in_order(turn, order):
    phase = order[-1]
    for index in range(len(order) - 2, -1, -1):
        phase = jnp.where(turn == index, order[index], phase)
    return phase


def settle(ref, sem):
    pltpu.make_async_copy(ref, ref, sem).wait()


def other_plane(plane, phase):
    turn = PHASES - 1 - phase
    high = lax.rem(plane // 2 + turn // 2, 2)
    low = lax.rem(plane + turn, 2)
    return high * 2 + low


def mixer_stage(
    count,
    docs,
    me,
    tp_rank,
    pool_ref,
    docs_ref,
    weights_ref,
    pool_gain_ref,
    padded,
    packed,
    unpacked,
    edge_docs,
    table,
    tables,
    pooled,
    edge_send,
    edge_recv,
    table_send,
    table_recv,
    spread,
):
    length, part = pool_ref.shape
    reach = length // 2
    barrier = pltpu.get_barrier_semaphore()
    own_rows = pltpu.make_async_copy(pool_ref, padded.at[pl.ds(reach, length)], edge_recv.at[6])
    own_rows.start()
    own_docs = jnp.concatenate([docs_ref[0], docs_ref[1]], axis=1).astype(jnp.float32)
    group_dim = weights_ref.shape[1]
    low, high = slice(0, LANES), slice(part - LANES, part)
    hot = (
        lax.broadcasted_iota(jnp.int32, (docs, length), 0).astype(jnp.float32) == own_docs
    ).astype(jnp.float32)
    sums = jnp.dot(
        hot.astype(jnp.bfloat16), pool_ref[:, high], preferred_element_type=jnp.float32
    )
    global_lane = lax.broadcasted_iota(jnp.int32, (docs, LANES), 1) >= LANES - group_dim
    table[...] = jnp.where(global_lane, sums, jnp.sum(hot, axis=1, keepdims=True))
    deep = reach // 2
    front = lax.broadcasted_iota(jnp.int32, (deep, LANES), 1) < group_dim
    for side, start in enumerate((length - reach, 0)):
        first = pool_ref[pl.ds(start, deep), high].astype(jnp.float32)
        second = pool_ref[pl.ds(start + deep, deep), high].astype(jnp.float32)
        packed[side] = jnp.where(
            front, first, pltpu.roll(second, group_dim, 1)
        ).astype(jnp.bfloat16)
    local_copy = pltpu.make_async_copy(table, tables.at[me], table_recv.at[0])
    local_copy.start()
    pl.semaphore_wait(barrier, count)
    right, left = lax.rem(me + 1, count), lax.rem(me + count - 1, count)
    copies = []
    for side, target in enumerate((right, left)):
        start = length - deep if side == 0 else 0
        into = reach - deep if side == 0 else reach + length
        for nth, (source, place) in enumerate(
            (
                (
                    pool_ref.at[pl.ds(start, deep), low],
                    padded.at[pl.ds(into, deep), low],
                ),
                (packed.at[side], unpacked.at[side]),
                (docs_ref.at[1 - side], edge_docs.at[side]),
            )
        ):
            copies.append(
                pltpu.make_async_remote_copy(
                    source,
                    place,
                    edge_send.at[3 * side + nth],
                    edge_recv.at[3 * side + nth],
                    device_id={"sp": target},
                )
            )

    def table_copy(step):
        return pltpu.make_async_remote_copy(
            table,
            tables.at[me],
            table_send.at[0],
            table_recv.at[0],
            device_id={"sp": lax.rem(me + step, count)},
        )

    for copy in copies:
        copy.start()

    def start_table(step, carry):
        table_copy(step).start()
        return carry

    lax.fori_loop(1, count, start_table, 0)
    spread()

    local_groups = part // weights_ref.shape[1]
    bands = []
    for group in range(local_groups):
        own = weights_ref[tp_rank * local_groups + group]
        pieces = [jnp.zeros_like(own)] * local_groups
        pieces[group] = own
        bands.append(jnp.concatenate(pieces, axis=1))
    block_weight = jnp.concatenate(bands, axis=0)
    all_gain = pool_gain_ref[...].astype(jnp.float32).reshape(1, -1)
    gain = all_gain[:, :part]
    for other in range(1, all_gain.shape[1] // part):
        rest = all_gain[:, other * part : (other + 1) * part]
        gain = jnp.where(tp_rank == other, rest, gain)
    own_column = jnp.transpose(jnp.broadcast_to(own_docs, (LANES, length)))[:, :1]
    block = length // 4
    lane_group = lax.broadcasted_iota(jnp.int32, (block, LANES), 1) // group_dim
    first_half = lane_group == 0
    own_rows.wait()
    for copy in copies:
        copy.wait()
    for side, start in enumerate((0, reach + length)):
        both = unpacked[side]
        padded[pl.ds(start, deep), high] = both
        padded[pl.ds(start + deep, deep), high] = pltpu.roll(
            both.astype(jnp.float32), LANES - group_dim, 1
        ).astype(jnp.bfloat16)
    before = jnp.where(me == 0, -1.0, edge_docs[0].astype(jnp.float32))
    after = jnp.where(me == count - 1, -1.0, edge_docs[1].astype(jnp.float32))
    all_docs = jnp.concatenate([before, own_docs, after], axis=1)

    settle(tables, table_recv.at[0])
    totals = jnp.sum(tables[...], axis=0)
    doc_means = totals / totals[:, :1]
    for index in range(length // block):
        rows = slice(index * block, (index + 1) * block)
        column = own_column[rows]

        def window_mean(level, columns):
            half_width = length * (1 << level) // 8
            span = block + 2 * half_width
            start = reach + index * block - half_width
            offsets = (
                lax.broadcasted_iota(jnp.int32, (block, span), 1)
                - half_width
                - lax.broadcasted_iota(jnp.int32, (block, span), 0)
            )
            reached = slice(start, start + span)
            inside = (
                (all_docs[:, reached] == column)
                & (offsets >= -half_width)
                & (offsets < half_width)
            )
            mask = jnp.where(inside, 1.0, 0.0)
            sums = jnp.dot(
                mask.astype(jnp.bfloat16),
                padded[reached, columns],
                preferred_element_type=jnp.float32,
            )
            return sums / jnp.sum(mask, axis=1, keepdims=True)

        doc_mean = jnp.zeros((block, LANES), jnp.float32)
        for doc in range(docs):
            doc_mean = jnp.where(column == doc, doc_means[doc : doc + 1], doc_mean)
        mean = jnp.concatenate(
            [
                jnp.where(first_half, window_mean(0, low), window_mean(1, low)),
                jnp.where(first_half, window_mean(2, high), doc_mean),
            ],
            axis=1,
        )
        difference = (mean - pool_ref[rows].astype(jnp.float32)).astype(jnp.bfloat16)
        pooled[rows] = (
            jnp.dot(difference, block_weight, preferred_element_type=jnp.float32) * gain
        ).astype(jnp.bfloat16)

    settle(tables.at[pl.ds(0, count - 1)], table_send.at[0])


def route(group_ref, experts_ref, share_ref, cap, slots, place, pick, share_send):
    rows = group_ref.shape[1]
    ids = group_ref[...]
    names = lax.broadcasted_iota(jnp.int32, (LANES, rows), 0)
    member = (ids == names).astype(jnp.float32)
    earlier = (
        lax.broadcasted_iota(jnp.int32, (rows, rows), 0)
        < lax.broadcasted_iota(jnp.int32, (rows, rows), 1)
    ).astype(jnp.float32)
    ahead = jnp.dot(
        member.astype(jnp.bfloat16),
        earlier.astype(jnp.bfloat16),
        preferred_element_type=jnp.float32,
    )
    rank = jnp.sum(ahead * member, axis=0, keepdims=True)
    slot = ids.astype(jnp.float32) * cap + rank
    chosen = (
        slot == lax.broadcasted_iota(jnp.int32, (slots, rows), 0).astype(jnp.float32)
    ).astype(jnp.float32)
    pick[...] = jnp.transpose(chosen).astype(jnp.bfloat16)
    place[...] = chosen.astype(jnp.bfloat16)
    spot = lax.broadcasted_iota(jnp.int32, (LANES, rows), 0)
    named = spot // cap
    total = jnp.zeros((LANES, rows), jnp.float32)
    for nth in range(experts_ref.shape[0]):
        here = experts_ref[nth : nth + 1] == named
        total = total + jnp.where(here, share_ref[nth : nth + 1].astype(jnp.float32), 0.0)
    total = jnp.where(rank == lax.rem(spot, cap).astype(jnp.float32), total, 0.0)
    sent = lax.dot_general(
        member.astype(jnp.bfloat16),
        total.astype(jnp.bfloat16),
        (((1,), (1,)), ((), ())),
        preferred_element_type=jnp.float32,
    )
    for dest in range(slots // cap):
        share_send[dest] = sent[dest : dest + 1]


def scaled(values, gain):
    return values * lax.rsqrt(jnp.mean(values * values, axis=-1, keepdims=True) + EPSILON) * gain


def layer_kernel(
    count,
    docs,
    pool_ref,
    docs_ref,
    residual_hbm,
    weights_ref,
    pool_gain_ref,
    output_hbm,
    mixer_gain_ref,
    routed_gain_ref,
    final_gain_ref,
    group_ref,
    experts_ref,
    share_ref,
    gate_hbm,
    up_hbm,
    down_hbm,
    out_hbm,
    padded,
    packed,
    unpacked,
    edge_docs,
    table,
    tables,
    pooled,
    swapped,
    output_weight,
    residual,
    mixed,
    stream,
    wide,
    place,
    pick,
    share_send,
    arrived_share,
    early_send,
    early_recv,
    pooled_send,
    pooled_recv,
    far_mixed,
    send_ref,
    fetched,
    arrived,
    gates,
    ups,
    downs,
    hidden,
    kept,
    outgoing,
    incoming,
    result,
    slot_stream,
    final,
    edge_send,
    edge_recv,
    table_send,
    table_recv,
    swap_sem,
    spread_send,
    spread_recv,
    weight_sem,
    send_sem,
    recv_sem,
    forward_send,
    forward_recv,
    part_send,
    part_recv,
    back_send,
    back_recv,
    first_send,
    first_recv,
    second_send,
    second_recv,
    write_sem,
):
    me, tp_rank = lax.axis_index("sp"), lax.axis_index("tp")
    per = count // PHASES
    plane, spot_of = me // per, lax.rem(me, per)
    rows, width = out_hbm.shape
    slots = send_ref.shape[0]
    cap = slots // count
    experts, _, units = gates.shape
    half = per * cap
    part = pool_ref.shape[1]
    greet()

    def block(index):
        return pl.ds(pl.multiple_of(index * cap, cap), cap)

    def target(step):
        phase = step // per
        spot = lax.rem(step + spot_of, per)
        return phase, spot, other_plane(plane, phase) * per + spot

    residual_load = pltpu.make_async_copy(residual_hbm, residual, weight_sem.at[4])
    output_load = pltpu.make_async_copy(output_hbm, output_weight, weight_sem.at[3])
    loads = [
        pltpu.make_async_copy(gate_hbm, gates, weight_sem.at[0]),
        pltpu.make_async_copy(up_hbm, ups, weight_sem.at[1]),
        pltpu.make_async_copy(down_hbm, downs, weight_sem.at[2]),
    ]
    for load in [residual_load, output_load] + loads:
        load.start()
    route(group_ref, experts_ref, share_ref, cap, slots, place, pick, share_send)
    tile = width // 4
    tiles = [slice(index * tile, (index + 1) * tile) for index in range(4)]

    def far_dest(step):
        return other_plane(plane, 0) * per + lax.rem(step + spot_of, per)

    far_place = jnp.concatenate([place[block(far_dest(step))] for step in range(EARLY)], axis=0)
    residual_load.wait()
    for columns in tiles:
        early_send[:, columns] = jnp.dot(
            far_place, residual[:, columns], preferred_element_type=jnp.float32
        ).astype(jnp.bfloat16)

    def far_copies(step):
        here = pl.ds(step * cap, cap)
        return [
            pltpu.make_async_remote_copy(
                source.at[here],
                into.at[here],
                send.at[0],
                recv.at[0],
                device_id={"sp": far_dest(step)},
            )
            for source, into, send, recv in (
                (early_send, early_recv, first_send, first_recv),
                (pooled_send, pooled_recv, second_send, second_recv),
            )
        ]

    far = [far_copies(step) for step in range(EARLY)]

    def share_copy(step):
        phase, _, dest = target(step)
        return dest, pltpu.make_async_remote_copy(
            share_send.at[dest],
            arrived_share.at[phase, 0, spot_of],
            spread_send.at[0],
            spread_recv.at[0],
            device_id={"sp": dest},
        )

    def spread():
        pltpu.make_async_copy(
            share_send.at[me],
            arrived_share.at[PHASES - 1, 0, spot_of],
            spread_recv.at[0],
        ).start()

        def start_share(step, carry):
            dest, copy = share_copy(step)

            @pl.when(dest != me)
            def _():
                copy.start()

            return carry

        lax.fori_loop(0, count, start_share, 0)
        for first, _ in far:
            first.start()

    mixer_stage(
        count,
        docs,
        me,
        tp_rank,
        pool_ref,
        docs_ref,
        weights_ref,
        pool_gain_ref,
        padded,
        packed,
        unpacked,
        edge_docs,
        table,
        tables,
        pooled,
        edge_send,
        edge_recv,
        table_send,
        table_recv,
        spread,
    )
    trade = pltpu.make_async_remote_copy(
        pooled.at[pl.ds(pl.multiple_of((1 - tp_rank) * rows, rows), rows)],
        swapped,
        swap_sem.at[0],
        swap_sem.at[1],
        device_id={"tp": 1 - tp_rank},
    )
    trade.start()
    output_load.wait()
    own_part = pooled[pl.ds(pl.multiple_of(tp_rank * rows, rows), rows)]
    own_from = pl.ds(pl.multiple_of(tp_rank * part, part), part)
    peer_from = pl.ds(pl.multiple_of((1 - tp_rank) * part, part), part)
    pooled_send[:, own_from] = jnp.dot(
        far_place, own_part, preferred_element_type=jnp.float32
    ).astype(jnp.bfloat16)
    for columns in tiles:
        mixed[:, columns] = jnp.dot(
            own_part, output_weight[own_from, columns], preferred_element_type=jnp.float32
        )
    trade.wait()
    pooled_send[:, peer_from] = jnp.dot(
        far_place, swapped[...], preferred_element_type=jnp.float32
    ).astype(jnp.bfloat16)
    for _, second in far:
        second.start()
    for columns in tiles:
        mixed[:, columns] += jnp.dot(
            swapped[...], output_weight[peer_from, columns], preferred_element_type=jnp.float32
        )
    mixer_gain = mixer_gain_ref[...].astype(jnp.float32).reshape(1, -1)
    routed_gain = routed_gain_ref[...].astype(jnp.float32).reshape(1, -1)
    final_gain = final_gain_ref[...].astype(jnp.float32).reshape(1, -1)
    chunk = min(128, half)

    def normalise(index, carry):
        here = pl.ds(pl.multiple_of(index * chunk, chunk), chunk)
        value = (
            residual[here].astype(jnp.float32) + scaled(mixed[here], mixer_gain)
        ).astype(jnp.bfloat16)
        stream[here] = value
        wide[here] = scaled(value.astype(jnp.float32), routed_gain).astype(jnp.bfloat16)
        return carry

    lax.fori_loop(0, rows // chunk, normalise, 0)
    def dispatch(step):
        phase = step // per
        spot = lax.rem(step + spot_of, per)
        dest = other_plane(plane, phase) * per + spot
        return dest, pltpu.make_async_remote_copy(
            send_ref.at[block(dest)],
            arrived.at[phase, block(spot_of)],
            send_sem.at[phase],
            recv_sem.at[phase],
            device_id={"sp": dest},
        )

    own_in = pltpu.make_async_copy(
        send_ref.at[block(me)],
        arrived.at[PHASES - 1, block(spot_of)],
        recv_sem.at[PHASES - 1],
    )

    def start_dispatch(step, carry):
        dest, copy = dispatch(step)

        @pl.when(dest != me)
        def _():
            copy.start()

        return carry

    for phase in SEND_ORDER:
        there = pl.ds(pl.multiple_of(other_plane(plane, phase) * half, half), half)
        for columns in tiles:
            send_ref[there, columns] = jnp.dot(
                place[there], wide[:, columns], preferred_element_type=jnp.float32
            ).astype(jnp.bfloat16)
        begin = EARLY if phase == 0 else phase * per
        lax.fori_loop(begin, (phase + 1) * per, start_dispatch, 0)
        if phase == PHASES - 1:
            own_in.start()

    for phase in range(PHASES):
        there = pl.ds(phase * half, half)
        for columns in tiles:
            slot_stream[there, columns] = jnp.dot(
                place[there], stream[:, columns], preferred_element_type=jnp.float32
            ).astype(jnp.bfloat16)

    settle(arrived_share.at[:, 0], spread_recv.at[0])
    share_forward = pltpu.make_async_remote_copy(
        arrived_share.at[:, 0],
        arrived_share.at[:, 1],
        swap_sem.at[2],
        swap_sem.at[3],
        device_id={"tp": 1 - tp_rank},
    )
    share_forward.start()
    for load in loads:
        load.wait()
    share_forward.wait()

    def back(step):
        phase = step // per
        spot = lax.rem(step + spot_of, per)
        dest = other_plane(plane, phase) * per + spot
        return dest, spot, pltpu.make_async_remote_copy(
            result.at[phase, block(spot)],
            fetched.at[block(me)],
            back_send.at[0],
            back_recv.at[phase],
            device_id={"sp": dest},
        )

    own_back = pltpu.make_async_copy(
        result.at[PHASES - 1, block(spot_of)], fetched.at[block(me)], back_recv.at[PHASES - 1]
    )

    def meet_far():
        settle(early_recv, first_recv.at[0])
        settle(pooled_recv, second_recv.at[0])
        for columns in tiles:
            far_mixed[:, columns] = jnp.dot(
                pooled_recv[...], output_weight[:, columns], preferred_element_type=jnp.float32
            )
        for step in range(EARLY):
            here = pl.ds(step * cap, cap)
            value = (
                early_recv[here].astype(jnp.float32) + scaled(far_mixed[here], mixer_gain)
            ).astype(jnp.bfloat16)
            arrived[0, block(lax.rem(spot_of + per - step, per))] = scaled(
                value.astype(jnp.float32), routed_gain
            ).astype(jnp.bfloat16)

    def start_back(step, carry):
        dest, _, copy = back(step)

        @pl.when(dest != me)
        def _():
            copy.start()

        return carry

    def return_phase(phase):
        lax.fori_loop(phase * per, (phase + 1) * per, start_back, 0)

    def forward(phase):
        return pltpu.make_async_remote_copy(
            arrived.at[phase, pl.ds(0, half)],
            arrived.at[phase, pl.ds(half, half)],
            forward_send.at[phase],
            forward_recv.at[phase],
            device_id={"tp": 1 - tp_rank},
        )

    def land(phase):
        @pl.when(phase == 0)
        def _():
            if EARLY < per:
                settle(arrived.at[0, pl.ds(0, half - EARLY * cap)], recv_sem.at[0])
            meet_far()

        @pl.when(phase != 0)
        def _():
            settle(arrived.at[phase, pl.ds(0, half)], recv_sem.at[phase])

        forward(phase).start()

    def swap(phase, index):
        columns = tiles[index]
        return pltpu.make_async_remote_copy(
            outgoing.at[phase, :, columns],
            incoming.at[phase, :, columns],
            part_send.at[phase],
            part_recv.at[phase],
            device_id={"tp": 1 - tp_rank},
        )

    land(SERVE_ORDER[0])

    def serve(turn, carry):
        phase = in_order(turn, SERVE_ORDER)
        later = in_order(turn, SERVE_ORDER[1:] + (0,))
        pieces = [arrived_share[phase, core, spot] for core in range(2) for spot in range(per)]
        pieces.append(jnp.zeros((LANES - 2 * per, LANES), jnp.float32))
        turned = jnp.transpose(jnp.concatenate(pieces, axis=0))
        forward(phase).wait()

        @pl.when(turn == EAGER)
        def _():
            land(later)

        for expert in range(experts):
            given = arrived[phase]
            gate = jnp.dot(given, gates[expert], preferred_element_type=jnp.float32)
            upper = jnp.dot(given, ups[expert], preferred_element_type=jnp.float32)
            silu = gate / (1.0 + jnp.exp(-gate))
            span = slice(expert * cap, (expert + 1) * cap)
            share = jnp.concatenate(
                [turned[span, column : column + 1] for column in range(2 * per)], axis=0
            )
            weighted = silu * upper * share
            hidden[:, expert * units : (expert + 1) * units] = weighted.astype(jnp.bfloat16)
        for index, columns in enumerate(tiles):
            product = jnp.dot(hidden[...], downs[:, columns], preferred_element_type=jnp.float32)
            kept[:, columns] = product[:half]
            outgoing[phase, :, columns] = product[half:].astype(jnp.bfloat16)
            swap(phase, index).start()

        @pl.when((turn != EAGER) & (turn < PHASES - 1))
        def _():
            land(later)

        settle(outgoing.at[phase], part_send.at[phase])
        settle(incoming.at[phase], part_recv.at[phase])
        for columns in tiles:
            result[phase, :, columns] = (
                kept[:, columns] + incoming[phase, :, columns].astype(jnp.float32)
            ).astype(jnp.bfloat16)

        @pl.when(turn == HOLDTURN)
        def _():
            settle(send_ref.at[pl.ds(0, half)], send_sem.at[1])
            return_phase(0)

        @pl.when(phase != 0)
        def _():
            return_phase(phase)

        return carry

    lax.fori_loop(0, PHASES, serve, 0)
    own_back.start()

    for phase in FINISH_ORDER:
        origin = other_plane(plane, phase)

        def update(index, carry):
            here = pl.ds(pl.multiple_of(origin * half + index * chunk, chunk), chunk)
            slot_stream[here] = (
                slot_stream[here].astype(jnp.float32)
                + scaled(fetched[here].astype(jnp.float32), final_gain)
            ).astype(jnp.bfloat16)
            return carry

        settle(fetched.at[pl.ds(0, half)], back_recv.at[phase])
        lax.fori_loop(0, half // chunk, update, 0)
    writes = []
    for index, columns in enumerate(tiles):
        final[:, columns] = jnp.dot(
            pick[...], slot_stream[:, columns], preferred_element_type=jnp.float32
        ).astype(jnp.bfloat16)
        writes.append(
            pltpu.make_async_copy(
                final.at[:, columns], out_hbm.at[:, columns], write_sem.at[index]
            )
        )
        writes[-1].start()
    settle(early_send, first_send.at[0])
    settle(pooled_send, second_send.at[0])
    settle(share_send.at[pl.ds(0, count - 1)], spread_send.at[0])
    settle(fetched.at[pl.ds(0, (count - 1) * cap)], back_send.at[0])
    for phase, blocks in ((0, per - EARLY), (2, per), (3, per - 1)):
        settle(send_ref.at[pl.ds(0, blocks * cap)], send_sem.at[phase])
    for write in writes:
        write.wait()


def local(
    pool_input,
    documents,
    residual,
    group_weights,
    pool_gain,
    output_weight,
    mixer_gain,
    routed_gain,
    final_gain,
    chosen_group,
    chosen_experts,
    expert_share,
    expert_gate,
    expert_up,
    expert_down,
):
    count = lax.axis_size("sp")
    docs = count // 4
    rows, width = residual.shape
    length, part = pool_input.shape
    reach = length // 2
    cap = length // count
    slots = count * cap
    per = count // PHASES
    half = per * cap
    down = expert_down.reshape(-1, width)
    bf16, f32 = jnp.bfloat16, jnp.float32
    dma, vmem = pltpu.SemaphoreType.DMA, pltpu.VMEM
    whole = pl.BlockSpec(memory_space=pltpu.VMEM)
    outside = pl.BlockSpec(memory_space=pl.ANY)
    return pl.pallas_call(
        functools.partial(layer_kernel, count, docs),
        out_shape=jax.ShapeDtypeStruct((rows, width), bf16),
        in_specs=[whole, whole, outside, whole, whole, outside]
        + [whole] * 6
        + [outside] * 3,
        out_specs=outside,
        scratch_shapes=[
            vmem((length + 2 * reach, part), bf16),
            vmem((2, reach // 2, LANES), bf16),
            vmem((2, reach // 2, LANES), bf16),
            vmem((2, 1, reach), documents.dtype),
            vmem((docs, LANES), f32),
            vmem((count, docs, LANES), f32),
            vmem((length, part), bf16),
            vmem((rows, part), bf16),
            vmem(output_weight.shape, bf16),
            vmem((rows, width), bf16),
            vmem((rows, width), f32),
            vmem((rows, width), bf16),
            vmem((rows, width), bf16),
            vmem((slots, rows), bf16),
            vmem((rows, slots), bf16),
            vmem((count, 1, LANES), f32),
            vmem((PHASES, 2, per, 1, LANES), f32),
            vmem((EARLY * cap, width), bf16),
            vmem((EARLY * cap, width), bf16),
            vmem((EARLY * cap, 2 * part), bf16),
            vmem((EARLY * cap, 2 * part), bf16),
            vmem((EARLY * cap, width), f32),
            vmem((slots, width), bf16),
            vmem((slots, width), bf16),
            vmem((PHASES, 2 * half, width), bf16),
            vmem(expert_gate.shape, bf16),
            vmem(expert_up.shape, bf16),
            vmem(down.shape, bf16),
            vmem((2 * half, down.shape[0]), bf16),
            vmem((half, width), f32),
            vmem((PHASES, half, width), bf16),
            vmem((PHASES, half, width), bf16),
            vmem((PHASES, half, width), bf16),
            vmem((slots, width), bf16),
            vmem((rows, width), bf16),
            dma((6,)),
            dma((7,)),
            dma((1,)),
            dma((1,)),
            dma((4,)),
            dma((1,)),
            dma((1,)),
            dma((5,)),
            dma((PHASES,)),
            dma((PHASES,)),
            dma((PHASES,)),
            dma((PHASES,)),
            dma((PHASES,)),
            dma((PHASES,)),
            dma((1,)),
            dma((PHASES,)),
            dma((1,)),
            dma((1,)),
            dma((1,)),
            dma((1,)),
            dma((4,)),
        ],
        compiler_params=pltpu.CompilerParams(
            collective_id=0, has_side_effects=True, vmem_limit_bytes=60 * 1024 * 1024
        ),
    )(
        pool_input,
        documents.reshape(2, 1, reach),
        residual,
        group_weights,
        pool_gain,
        output_weight,
        mixer_gain,
        routed_gain,
        final_gain,
        chosen_group.T,
        chosen_experts.T,
        expert_share.T,
        expert_gate,
        expert_up,
        down,
    )


def solution(mesh):
    placed = (
        P("sp", "tp"),
        P("sp"),
        P(("sp", "tp"), None),
        P(),
        P(),
        P(),
        P(),
        P(),
        P(),
        P(("sp", "tp"), None),
        P(("sp", "tp"), None),
        P(("sp", "tp"), None),
        P("sp", None, "tp"),
        P("sp", None, "tp"),
        P("sp", "tp", None),
    )
    return jax.shard_map(
        local, mesh=mesh, in_specs=placed, out_specs=P(("sp", "tp"), None), check_vma=False
    )
```
